32 devices in a mesh: sp: 4 (over y, x), tp: 8 (over z, core).
Axes of the slice: x: 2, y: 2, z: 4, core: 2. Of those that a mesh axis runs over, the one named last changes fastest.
Arguments:
- conv_outer: bfloat16 [2048, 1024], P('tp', 'sp'), may hold values from -6 to 6
- conv_inner: bfloat16 [2048, 1024], P('tp', 'sp'), may hold values from -6 to 6
- conv_input: bfloat16 [2048, 1024], P('tp', 'sp'), may hold values from -6 to 6
- conv_taps: float32 [3, 2048], P(None, 'tp'), may hold values from -3 to 3
- out_proj: bfloat16 [2048, 4096], P('tp'), may hold values from -0.125 to 0.125
- mixed_state: bfloat16 [1024, 4096], P('sp', 'tp'), may hold values from -6 to 6
- route_ids: int32 [1024, 2], P('sp'), may hold values from 0 to 3, all different within a row; in each aligned block of 256 rows (0 to 255, 256 to 511, ...) at most 256 rows name the same one
- route_weights: float32 [1024, 2], P('sp'), may hold values from 0.1 to 1
- w_gate: bfloat16 [4, 2048, 4096], P('sp', 'tp'), may hold values from -0.09375 to 0.09375
- w_up: bfloat16 [4, 2048, 4096], P('sp', 'tp'), may hold values from -0.09375 to 0.09375
- w_down: bfloat16 [4, 2048, 4096], P('sp', 'tp'), may hold values from -0.125 to 0.125
- cotangent: bfloat16 [1024, 4096], P('sp', 'tp'), may hold values from -8 to 8
Outputs:
- grad_gate: float32 [4, 2048, 4096], P('sp', 'tp')
- grad_up: float32 [4, 2048, 4096], P('sp', 'tp')
- grad_down: float32 [4, 2048, 4096], P('sp', 'tp')
- grad_mixed: bfloat16 [1024, 4096], P('sp', 'tp')
- grad_proj: float32 [2048, 4096], P('tp', 'sp')
- grad_outer: bfloat16 [2048, 1024], P('tp', 'sp')
- grad_inner: bfloat16 [2048, 1024], P('tp', 'sp')
- grad_input: bfloat16 [2048, 1024], P('tp', 'sp')
The draws below stay inside these ranges and needn't reach their ends.
Inputs may be any that keep to these rules, and one draw needn't show every extreme that they name: `route_ids`: each row names 2 different experts; among the tokens of one index of sp no expert is named more than 256 times, a bound that some block reaches.
All inputs are finite; a program needn't handle non-finite values.
Results may differ from the reference program's by a relative error of at most 0.022.
Values may be sent and summed in bfloat16 or wider, within the bound.
A program may use at most 128 MiB of HBM per device.

```python
import math
import jax
import jax.numpy as jnp
import numpy as np
from jax import lax

D = 4096
FF = 2048
CH = 2048
TAPS = 3
TOP = 2
TOK_DEV = 256
EXPERTS = 4
CAP = 256
TOKENS = 1024
N_SP = 4
N_TP = 8


def with_spikes(result, rng, source, target, blocks, factor):
    def block_of(dim):
        return (jnp.arange(result.shape[dim]) // (result.shape[dim] // blocks)).reshape((-1,) + (1,) * (result.ndim - 1 - dim))

    near = jax.random.permutation(rng, blocks)[block_of(target)]
    other_side = (block_of(target) + blocks // 2) % blocks
    return jnp.where((block_of(source) == near) | (block_of(source) == other_side), factor * result, result)


def level_of(stream_key, dims, cuts, least, top_value):
    def one(axis_at, shards_of):
        heights = jax.random.uniform(jax.random.fold_in(jax.random.fold_in(stream_key, 6), axis_at), (shards_of,), jnp.float32, least / len(cuts), top_value / len(cuts))
        return jnp.repeat(jnp.exp(heights), dims[axis_at] // shards_of).reshape((-1,) + (1,) * (len(dims) - axis_at - 1))

    factor_of = one(*cuts[0])
    for cut in cuts[1:]:
        factor_of = factor_of * one(*cut)
    return factor_of


def shared_out(stream_key, own, number, rows, amount, top, most, lean):
    ranking = jax.random.permutation(stream_key, amount)
    packed, ordinary = load_shares(amount, rows * top, most, lean, True), load_shares(amount, rows * top, most, lean, False)
    places = jnp.arange(amount)

    def named(lengths, rotation):
        used = int((lengths > 0).sum())
        fixed = max(1, used // 4)
        shifted = fixed + (places - fixed + rotation * (used - fixed)) % max(1, amount - fixed)
        return jnp.zeros((amount,), jnp.int32).at[ranking[jnp.where(places < fixed, places, shifted)]].set(jnp.asarray(lengths, jnp.int32))

    lengths = jnp.where(number % 4 == 0, named(packed, number // 4), named(ordinary, number - number // 4 - 1))
    mixed = jax.random.permutation(jax.random.fold_in(own, 3), amount)
    giver, taker = mixed[0:amount // 2 * 2:2], mixed[1:amount // 2 * 2:2]
    margin = jnp.minimum(lengths[giver] - 1, most - lengths[taker]) // 2
    margin = jnp.where((giver == ranking[0]) | (taker == ranking[0]) | (lengths[taker] == 0), 0, jnp.maximum(margin, 0))
    shifted = jax.random.randint(jax.random.fold_in(own, 4), (amount // 2,), 0, 1 << 20) % (margin + 1)
    lengths = lengths.at[giver].add(-shifted).at[taker].add(shifted)
    items = jnp.searchsorted(jnp.cumsum(lengths), jnp.arange(rows * top), side="right").astype(jnp.int32)
    grid = items.reshape(top, rows).T
    grid = grid[jax.random.permutation(jax.random.fold_in(own, 1), rows)]
    rotation = jax.random.randint(jax.random.fold_in(own, 2), (rows, 1), 0, top)
    return jnp.take_along_axis(grid, (jnp.arange(top)[None, :] + rotation) % top, axis=1)


def load_shares(number_of, total, most, slope, full):
    loads = [(1 << 20) // math.isqrt(standing ** slope) + 1 for standing in range(1, number_of + 1)]
    largest = most if full else min(most, max(-(-total // number_of), total * loads[0] // sum(loads)))
    least = 1 if total - largest >= number_of - 1 else 0
    holding, surplus = [largest] + [least] * (number_of - 1), total - largest - least * (number_of - 1)
    while surplus > 0:
        free = [i for i in range(1, number_of) if holding[i] < largest] or [i for i in range(1, number_of) if holding[i] < most]
        pool, left = sum([loads[i] for i in free]), surplus
        for i in free:
            extra = min(most - holding[i], max(1, left * loads[i] // pool), surplus)
            holding[i] = holding[i] + extra
            surplus = surplus - extra
    return np.array(holding)


def centred(key, extent, scale, limit, split=(), kind=jnp.bfloat16):
    values = jax.random.normal(key, extent, jnp.float32) * scale
    if len(split) > 0:
        values = level_of(key, extent, split, -0.22, 0.18) * values
    return jnp.clip(values, min=-limit, max=limit).astype(kind)


def noise_with(key, shape, spread, most, split, heavy, held_as=jnp.bfloat16):
    drawn = spread * jax.random.normal(key, shape, jnp.float32)
    if split:
        drawn = drawn * level_of(key, shape, split, -0.22, 0.18)
    return jnp.clip(with_spikes(drawn, jax.random.fold_in(key, 3), *heavy), -most, most).astype(held_as)


def setup_inputs(seed: int = 0) -> dict:
    arg_keys = jax.random.split(jax.random.key(seed), 13)
    conv_outer = centred(arg_keys[0], (CH, TOKENS), 1.0, 6.0, ((0, 8), (1, 4)))
    conv_inner = centred(arg_keys[1], (CH, TOKENS), 1.0, 6.0, ((0, 8), (1, 4)))
    conv_input = centred(arg_keys[2], (CH, TOKENS), 1.0, 6.0, ((0, 8), (1, 4)))
    conv_taps = centred(arg_keys[3], (TAPS, CH), 0.6, 3.0, ((1, 8),), jnp.float32)
    out_proj = centred(arg_keys[4], (CH, D), CH ** -0.5, 0.125, ((0, 8),))
    mixed_state = centred(arg_keys[5], (TOKENS, D), 1.0, 6.0, ((0, 4), (1, 8)))
    route_ids_keys = jax.random.split(jax.random.fold_in(arg_keys[6], 1), TOKENS // TOK_DEV)
    route_ids_turns = jax.random.permutation(jax.random.fold_in(arg_keys[6], 3), TOKENS // TOK_DEV)
    route_ids = jax.vmap(lambda own, number: shared_out(jax.random.fold_in(arg_keys[6], 2), own, number, TOK_DEV, EXPERTS, TOP, CAP, 2))(route_ids_keys, route_ids_turns).reshape((TOKENS, TOP))
    route_weights = jnp.clip(0.1 + 0.9 * jax.random.uniform(arg_keys[7], (TOKENS, TOP), jnp.float32) ** level_of(arg_keys[7], (TOKENS, TOP), ((0, 4),), -0.2, 0.2), 0.1, 1.0)
    w_gate = centred(arg_keys[8], (EXPERTS, FF, D), D ** -0.5, 0.09375, ((0, 4), (1, 8)))
    w_up = centred(arg_keys[9], (EXPERTS, FF, D), D ** -0.5, 0.09375, ((0, 4), (1, 8)))
    w_down = centred(arg_keys[10], (EXPERTS, FF, D), FF ** -0.5, 0.125, ((0, 4), (1, 8)))
    cotangent = noise_with(arg_keys[11], (TOKENS, D), 1.0, 8.0, ((0, 4), (1, 8)), (0, 1, 8, 2.0))
    return {"conv_outer": conv_outer, "conv_inner": conv_inner, "conv_input": conv_input, "conv_taps": conv_taps, "out_proj": out_proj, "mixed_state": mixed_state, "route_ids": route_ids, "route_weights": route_weights, "w_gate": w_gate, "w_up": w_up, "w_down": w_down, "cotangent": cotangent}


def expert_core(rows_in, rows_grad, gate_w, up_w, down_w):
    gate_pre = jnp.dot(rows_in, gate_w.T, preferred_element_type=jnp.float32)
    up_pre = jnp.dot(rows_in, up_w.T, preferred_element_type=jnp.float32)
    sig_gate = jax.nn.sigmoid(gate_pre)
    silu_gate = gate_pre * sig_gate
    hidden = (silu_gate * up_pre).astype(jnp.bfloat16)
    back_hidden = jnp.dot(rows_grad, down_w.T, preferred_element_type=jnp.float32)
    back_gate = (back_hidden * up_pre * sig_gate * (1.0 + gate_pre * (1.0 - sig_gate))).astype(jnp.bfloat16)
    back_up = (back_hidden * silu_gate).astype(jnp.bfloat16)
    grad_down_e = jnp.dot(hidden.T, rows_grad, preferred_element_type=jnp.float32)
    grad_gate_e = jnp.dot(back_gate.T, rows_in, preferred_element_type=jnp.float32)
    grad_up_e = jnp.dot(back_up.T, rows_in, preferred_element_type=jnp.float32)
    return back_gate, back_up, grad_gate_e, grad_up_e, grad_down_e


def reference(conv_outer, conv_inner, conv_input, conv_taps, out_proj, mixed_state, route_ids, route_weights, w_gate, w_up, w_down, cotangent):
    block_ids = route_ids.reshape(N_SP, TOP * TOK_DEV)
    onehot = (block_ids[:, :, None] == jnp.arange(EXPERTS, dtype=jnp.int32)[None, None, :]).astype(jnp.int32)
    position = jnp.sum(jnp.cumsum(onehot, axis=1) * onehot, axis=2) - 1
    device_ids = jnp.broadcast_to(jnp.arange(N_SP, dtype=jnp.int32)[:, None], block_ids.shape)
    assign = jnp.arange(N_SP * TOP * TOK_DEV, dtype=jnp.int32).reshape(N_SP, TOP * TOK_DEV)
    table = jnp.full((EXPERTS, N_SP, CAP), -1, jnp.int32).at[block_ids, device_ids, position].set(assign)
    table = table.reshape(EXPERTS, N_SP * CAP)
    weight_flat = route_weights.reshape(-1)

    def expert_pass(operands):
        table_row, gate_w, up_w, down_w = operands
        valid = table_row >= 0
        safe_idx = jnp.where(valid, table_row, 0)
        token_idx = safe_idx // TOP
        rows_in = jnp.where(valid[:, None], mixed_state[token_idx], jnp.zeros((), jnp.bfloat16))
        scale = jnp.where(valid, weight_flat[safe_idx], jnp.zeros((), jnp.float32))
        rows_grad = (cotangent[token_idx].astype(jnp.float32) * scale[:, None]).astype(jnp.bfloat16)
        back_gate, back_up, grad_gate_e, grad_up_e, grad_down_e = expert_core(rows_in, rows_grad, gate_w, up_w, down_w)
        row_count = rows_in.shape[0]
        gate_blocks = back_gate.astype(jnp.float32).reshape(row_count, N_TP, FF // N_TP)
        up_blocks = back_up.astype(jnp.float32).reshape(row_count, N_TP, FF // N_TP)
        gate_wblk = gate_w.astype(jnp.float32).reshape(N_TP, FF // N_TP, D)
        up_wblk = up_w.astype(jnp.float32).reshape(N_TP, FF // N_TP, D)
        partial_value = jnp.einsum("rbf,bfd->brd", gate_blocks, gate_wblk) + jnp.einsum("rbf,bfd->brd", up_blocks, up_wblk)
        rounded = lax.optimization_barrier(partial_value.astype(jnp.bfloat16))
        row_back = jnp.sum(rounded.astype(jnp.float32), axis=0).astype(jnp.bfloat16)
        return row_back, grad_gate_e, grad_up_e, grad_down_e

    row_back, grad_gate, grad_up, grad_down = lax.map(expert_pass, (table, w_gate, w_up, w_down))
    flat_table = table.reshape(-1)
    valid_all = flat_table >= 0
    token_all = jnp.where(valid_all, flat_table, 0) // TOP
    back_vals = jnp.where(valid_all[:, None], row_back.reshape(-1, D).astype(jnp.float32), jnp.zeros((), jnp.float32))
    moe_grad = jnp.zeros((TOKENS, D), jnp.float32).at[token_all].add(back_vals)
    grad_mixed = (cotangent.astype(jnp.float32) + moe_grad).astype(jnp.bfloat16)

    inner_prod = conv_inner.astype(jnp.float32) * conv_input.astype(jnp.float32)
    padded = jnp.pad(inner_prod, ((0, 0), (TAPS - 1, 0)))
    conv_out = jnp.zeros_like(inner_prod)
    for offset in range(TAPS):
        conv_out = conv_out + conv_taps[offset][:, None] * padded[:, offset:offset + TOKENS]
    mixer_act = (conv_outer.astype(jnp.float32) * conv_out).astype(jnp.bfloat16)
    back_mixer = jnp.dot(out_proj, grad_mixed.T, preferred_element_type=jnp.float32)
    grad_proj = jnp.dot(mixer_act, grad_mixed, preferred_element_type=jnp.float32)
    grad_outer = (back_mixer * conv_out).astype(jnp.bfloat16)
    back_conv = back_mixer * conv_outer.astype(jnp.float32)
    padded_back = jnp.pad(back_conv, ((0, 0), (0, TAPS - 1)))
    back_prod = jnp.zeros_like(back_conv)
    for offset in range(TAPS):
        shift_by = TAPS - 1 - offset
        back_prod = back_prod + conv_taps[offset][:, None] * padded_back[:, shift_by:shift_by + TOKENS]
    grad_inner = (back_prod * conv_input.astype(jnp.float32)).astype(jnp.bfloat16)
    grad_input = (back_prod * conv_inner.astype(jnp.float32)).astype(jnp.bfloat16)
    return grad_gate, grad_up, grad_down, grad_mixed, grad_proj, grad_outer, grad_inner, grad_input
```

```python
import functools

import jax
import jax.numpy as jnp
from jax import lax
from jax.experimental import pallas as pl
from jax.experimental.pallas import tpu as pltpu
from jax.sharding import PartitionSpec as P


def from_behind(value, axis, steps):
    count = lax.axis_size(axis)
    first, last = (max(0, -steps), min(count, count - steps))
    return lax.ppermute(value, axis, [(source, source + steps) for source in range(first, last)])


def row_back_kernel(gate_ref, up_ref, gate_w_ref, up_w_ref, out_ref):
    total = jnp.dot(gate_ref[...], gate_w_ref[...], preferred_element_type=jnp.float32)
    total += jnp.dot(up_ref[...], up_w_ref[...], preferred_element_type=jnp.float32)
    out_ref[...] = total.astype(out_ref.dtype)


def row_back(back_gate, back_up, gate_w, up_w):
    rows, hidden = back_gate.shape
    width = gate_w.shape[1]
    tile = min(512, width)
    left = pl.BlockSpec((rows, hidden), lambda i: (0, 0))
    right = pl.BlockSpec((hidden, tile), lambda i: (0, i))
    return pl.pallas_call(
        row_back_kernel,
        grid=(width // tile,),
        out_shape=jax.ShapeDtypeStruct((rows, width), jnp.bfloat16),
        in_specs=[left, left, right, right],
        out_specs=pl.BlockSpec((rows, tile), lambda i: (0, i)),
        cost_estimate=pl.CostEstimate(
            flops=4 * rows * hidden * width,
            bytes_accessed=2 * (2 * rows * hidden + 2 * hidden * width + rows * width),
            transcendentals=0,
        ),
        name="row_back",
    )(back_gate, back_up, gate_w, up_w)


def expert_step(rows_in, rows_grad, gate_w, up_w, down_w):
    gate_pre = jnp.einsum("rd,fd->rf", rows_in, gate_w, preferred_element_type=jnp.float32)
    up_pre = jnp.einsum("rd,fd->rf", rows_in, up_w, preferred_element_type=jnp.float32)
    sig_gate = jax.nn.sigmoid(gate_pre)
    silu_gate = gate_pre * sig_gate
    hidden = (silu_gate * up_pre).astype(jnp.bfloat16)
    back_hidden = jnp.einsum("rd,fd->rf", rows_grad, down_w, preferred_element_type=jnp.float32)
    back_gate = (back_hidden * up_pre * sig_gate * (1.0 + gate_pre * (1.0 - sig_gate))).astype(
        jnp.bfloat16
    )
    back_up = (back_hidden * silu_gate).astype(jnp.bfloat16)
    grad_down_e = jnp.einsum("rf,rd->fd", hidden, rows_grad, preferred_element_type=jnp.float32)
    grad_gate_e = jnp.einsum("rf,rd->fd", back_gate, rows_in, preferred_element_type=jnp.float32)
    grad_up_e = jnp.einsum("rf,rd->fd", back_up, rows_in, preferred_element_type=jnp.float32)
    partial_value = row_back(back_gate, back_up, gate_w, up_w)
    return (partial_value, grad_gate_e, grad_up_e, grad_down_e)


Z_UP, Z_DOWN, BY_X, BY_Y, HALF_X, HALF_Y, PEER = range(7)
KINDS = PEER + 4


def gather_kernel(levels, cot_in, state_in, cot_out, state_out, own_sem, send_sem, recv_sem):
    sp, tp = lax.axis_index("sp"), lax.axis_index("tp")
    level, core = tp // 2, tp % 2
    beside_x = sp + 1 - 2 * (sp % 2)
    beside_y = (sp + 2) % 4
    across = 3 - sp
    peer = tp + 1 - 2 * core
    rows, cols = cot_in.shape
    half = rows // 2
    ins, outs = (cot_in, state_in), (cot_out, state_out)

    barrier = pltpu.get_barrier_semaphore()

    def greet(to_sp, to_tp):
        pl.semaphore_signal(
            barrier,
            inc=1,
            device_id=(to_sp, to_tp),
            device_id_type=pl.DeviceIdType.MESH,
        )

    greet(beside_x, tp)
    greet(beside_y, tp)
    greet(sp, peer)
    pl.when(level > 0)(lambda: greet(sp, tp - 2))
    pl.when(level < levels - 1)(lambda: greet(sp, tp + 2))
    one = jnp.int32(1)
    none = jnp.int32(0)
    pl.semaphore_wait(
        barrier,
        3 + jnp.where(level > 0, one, none) + jnp.where(level < levels - 1, one, none),
    )

    def block(array, of_sp, of_level, of_core, start=0, size=rows):
        return outs[array].at[
            pl.ds(pl.multiple_of(of_sp * rows + start, 16), size),
            pl.ds(pl.multiple_of((of_level * 2 + of_core) * cols, 128), cols),
        ]

    def remote(array, kind, of_level, source, target, to_sp, to_tp):
        return pltpu.make_async_remote_copy(
            src_ref=source,
            dst_ref=target,
            send_sem=send_sem.at[array, kind, of_level],
            recv_sem=recv_sem.at[array, kind, of_level],
            device_id=(to_sp, to_tp),
            device_id_type=pl.DeviceIdType.MESH,
        )

    def spread(array, of_level, source, kind, to_sp, to_tp):
        remote(
            array, kind, of_level, source, block(array, sp, of_level, core), to_sp, to_tp
        ).start()

    def pieces(array, of_level):
        return {
            Z_UP: block(array, sp, of_level, core),
            Z_DOWN: block(array, sp, of_level, core),
            BY_X: block(array, beside_x, of_level, core),
            BY_Y: block(array, beside_y, of_level, core),
            HALF_Y: block(array, across, of_level, core, 0, half),
            HALF_X: block(array, across, of_level, core, half, half),
            PEER: block(array, sp, of_level, 1 - core),
            PEER + 1: block(array, beside_x, of_level, 1 - core),
            PEER + 2: block(array, beside_y, of_level, 1 - core),
            PEER + 3: block(array, across, of_level, 1 - core),
        }

    def arrive(array, kind, of_level):
        piece = pieces(array, of_level)[kind]
        remote(array, kind, of_level, piece, piece, sp, peer).wait_recv()

    def left(array, kind, of_level):
        piece = pieces(array, of_level)[kind]
        remote(array, kind, of_level, piece, piece, sp, peer).wait_send()

    def hand_on(array, of_level, kind, of_sp, to_sp, to_tp, start=0, size=rows):
        piece = block(array, of_sp, of_level, core, start, size)
        remote(array, kind, of_level, piece, piece, to_sp, to_tp).start()

    def column(array, step, up):
        of_level = level if step == 0 else (level - step if up else level + step)
        if step == 0:
            source = ins[array]
            pltpu.make_async_copy(
                source, block(array, sp, level, core), own_sem.at[array]
            ).start()
        else:
            arrive(array, Z_UP if up else Z_DOWN, of_level)
            source = block(array, sp, of_level, core)
        if step == 0 or up:
            pl.when(level < levels - 1)(
                lambda: spread(array, of_level, source, Z_UP, sp, tp + 2)
            )
        if step == 0 or not up:
            pl.when(level > 0)(lambda: spread(array, of_level, source, Z_DOWN, sp, tp - 2))
        spread(array, of_level, source, BY_X, beside_x, tp)
        spread(array, of_level, source, BY_Y, beside_y, tp)
        spread(array, of_level, source, PEER, sp, peer)

    def plane(array, step, up):
        of_level = level - step if up else level + step
        arrive(array, BY_X, of_level)
        hand_on(array, of_level, HALF_Y, beside_x, beside_y, tp, 0, half)
        hand_on(array, of_level, PEER + 1, beside_x, sp, peer)
        arrive(array, BY_Y, of_level)
        hand_on(array, of_level, HALF_X, beside_y, beside_x, tp, half, half)
        hand_on(array, of_level, PEER + 2, beside_y, sp, peer)

    def corner(array, step, up):
        of_level = level - step if up else level + step
        arrive(array, HALF_X, of_level)
        arrive(array, HALF_Y, of_level)
        hand_on(array, of_level, PEER + 3, across, sp, peer)

    def each(action, step):
        if not 0 <= step < levels:
            return
        if step == 0:
            for array in range(2):
                action(array, 0, True)
            return

        @pl.when(level >= step)
        def _():
            for array in range(2):
                action(array, step, True)

        @pl.when(level < levels - step)
        def _():
            for array in range(2):
                action(array, step, False)

    for step in range(levels + 2):
        each(column, step)
        each(plane, step - 1)
        each(corner, step - 2)

    for array in range(2):
        pltpu.make_async_copy(
            ins[array], block(array, sp, level, core), own_sem.at[array]
        ).wait()
        for of_level in range(levels):
            for kind in (PEER, PEER + 1, PEER + 2, PEER + 3):
                arrive(array, kind, of_level)
                left(array, kind, of_level)
            for kind in (BY_X, BY_Y, HALF_X, HALF_Y):
                left(array, kind, of_level)
            pl.when((level < levels - 1) & (level >= of_level))(
                lambda: left(array, Z_UP, of_level)
            )
            pl.when((level > 0) & (level <= of_level))(lambda: left(array, Z_DOWN, of_level))


def gather_all(cotangent, mixed_state):
    rows, cols = cotangent.shape
    levels = lax.axis_size("tp") // 2
    whole = jax.ShapeDtypeStruct((4 * rows, 2 * levels * cols), cotangent.dtype)
    return pl.pallas_call(
        functools.partial(gather_kernel, levels),
        out_shape=(whole, whole),
        in_specs=[pl.BlockSpec(memory_space=pltpu.VMEM)] * 2,
        out_specs=[pl.BlockSpec(memory_space=pl.ANY)] * 2,
        scratch_shapes=[
            pltpu.SemaphoreType.DMA((2,)),
            pltpu.SemaphoreType.DMA((2, KINDS, levels)),
            pltpu.SemaphoreType.DMA((2, KINDS, levels)),
        ],
        compiler_params=pltpu.CompilerParams(collective_id=0, has_side_effects=True),
        name="gather_all",
    )(cotangent, mixed_state)


PIECES = 2
TO_X, TO_Y, PASS_X, PASS_Y, LAST_X, LAST_Y = range(6)


def level_at(level, place):
    inner = (0, 3, 1, 2)[place]
    high = jnp.where((level == 0) | (level == 3), place, inner)
    return jnp.where(level >= 2, high, 3 - high)


def reduce_kernel(
    back_in,
    gate_in,
    up_in,
    cot_in,
    act_in,
    own_out,
    token_out,
    quarter_out,
    act_out,
    back,
    weights,
    part,
    passed,
    landed,
    plane_sum,
    z_send,
    z_land,
    own_sem,
    swap_send,
    swap_recv,
    plane_send,
    plane_recv,
    chain_send,
    chain_recv,
    up_send,
    down_send,
    spread_recv,
    peer_send,
    peer_recv,
    quarter_send,
    quarter_recv,
    mate_send,
    mate_recv,
    act_send,
    act_recv,
):
    sp, tp = lax.axis_index("sp"), lax.axis_index("tp")
    level, core = tp // 2, tp % 2
    beside_x = sp + 1 - 2 * (sp % 2)
    beside_y = (sp + 2) % 4
    across = 3 - sp
    peer = tp + 1 - 2 * core
    levels = 4
    rows, half_cols = cot_in.shape
    cols = half_cols // PIECES
    half = rows // 2
    hidden = gate_in.shape[0]
    steps = PIECES * levels
    at_end = (level == 0) | (level == levels - 1)

    barrier = pltpu.get_barrier_semaphore()

    def greet(to_sp, to_tp):
        pl.semaphore_signal(
            barrier,
            inc=1,
            device_id=(to_sp, to_tp),
            device_id_type=pl.DeviceIdType.MESH,
        )

    greet(beside_x, tp)
    greet(beside_y, tp)
    greet(across, tp)
    greet(sp, peer)
    pl.when(level > 0)(lambda: greet(sp, tp - 2))
    pl.when(level < levels - 1)(lambda: greet(sp, tp + 2))
    pl.semaphore_wait(barrier, 6 - jnp.where(at_end, jnp.int32(1), jnp.int32(0)))

    sent = []

    def always(action):
        action()

    def remote(source, target, send, recv, to_sp, to_tp):
        return pltpu.make_async_remote_copy(
            src_ref=source,
            dst_ref=target,
            send_sem=send,
            recv_sem=recv,
            device_id=(to_sp, to_tp),
            device_id_type=pl.DeviceIdType.MESH,
        )

    def send(source, target, send_sem, recv_sem, to_sp, to_tp, when=always):
        def build():
            return remote(source, target, send_sem, recv_sem, to_sp, to_tp)

        when(lambda: build().start())
        sent.append((when, lambda: build().wait_send()))

    def arrive(piece, recv_sem):
        remote(piece, piece, act_send.at[0], recv_sem, sp, peer).wait_recv()

    mine = pl.ds(0, 2 * hidden)
    send(back_in, back.at[:, pl.ds(2 * hidden, 2 * hidden)], swap_send.at[0], swap_recv.at[0], sp, peer)
    pltpu.make_async_copy(back_in, back.at[:, mine], own_sem.at[0]).start()

    def own_weights(place, which):
        of_level = level_at(level, place)
        source = (gate_in, up_in)[which].at[
            :, pl.ds(pl.multiple_of((of_level * 2 + core) * half_cols, 128), half_cols)
        ]
        target = weights.at[place, pl.ds(which * hidden, hidden)]
        return pltpu.make_async_copy(source, target, own_sem.at[1 + 2 * place + which])

    for place in range(levels):
        for which in range(2):
            of_level = level_at(level, place)
            send(
                (gate_in, up_in)[which].at[
                    :, pl.ds(pl.multiple_of((of_level * 2 + 1 - core) * half_cols, 128), half_cols)
                ],
                weights.at[place, pl.ds((2 + which) * hidden, hidden)],
                swap_send.at[1 + 2 * place + which],
                swap_recv.at[1 + 2 * place + which],
                sp,
                peer,
            )
            own_weights(place, which).start()

    def block(step, of_sp, start, size):
        return part.at[step, pl.ds(pl.multiple_of(of_sp * rows + start, 128), size)]

    def plane(step, kind, source, to_sp):
        send(
            source,
            landed.at[step, kind],
            plane_send.at[step, kind],
            plane_recv.at[step, kind],
            to_sp,
            tp,
        )

    def form(step):
        piece, place = step // levels, step % levels
        if step < levels:
            for which in range(2):
                own_weights(place, which).wait()
                arrive(
                    weights.at[place, pl.ds((2 + which) * hidden, hidden)],
                    swap_recv.at[1 + 2 * place + which],
                )
        if step == 0:
            pltpu.make_async_copy(back_in, back.at[:, mine], own_sem.at[0]).wait()
            arrive(back.at[:, pl.ds(2 * hidden, 2 * hidden)], swap_recv.at[0])

        def one(at, _):
            span = pl.ds(pl.multiple_of(at * rows, 128), rows)
            part[step, span, :] = jnp.dot(
                back[span, :],
                weights[place, :, piece * cols : (piece + 1) * cols],
                preferred_element_type=jnp.float32,
            ).astype(part.dtype)
            return 0

        lax.fori_loop(0, 4, one, 0)
        plane(step, PASS_X, block(step, across, 0, half), beside_x)
        plane(step, PASS_Y, block(step, across, half, half), beside_y)
        plane(step, TO_X, block(step, beside_x, 0, half), beside_x)
        plane(step, TO_Y, block(step, beside_y, half, half), beside_y)

    def wide(value):
        return value.astype(jnp.float32)

    def hand_on(step):
        arrive(landed.at[step, PASS_X], plane_recv.at[step, PASS_X])
        passed[step, 0] = (
            wide(block(step, beside_y, 0, half)[...]) + wide(landed[step, PASS_X])
        ).astype(passed.dtype)
        plane(step, LAST_Y, passed.at[step, 0], beside_y)
        arrive(landed.at[step, PASS_Y], plane_recv.at[step, PASS_Y])
        passed[step, 1] = (
            wide(block(step, beside_x, half, half)[...]) + wide(landed[step, PASS_Y])
        ).astype(passed.dtype)
        plane(step, LAST_X, passed.at[step, 1], beside_x)

    def chain(step, when):
        piece, place = step // levels, step % levels
        of_level = level_at(level, place)
        upward = jnp.where(of_level > level, jnp.int32(1), jnp.int32(0))
        send(
            z_send.at[step],
            z_land.at[piece, of_level, 1 - upward],
            chain_send.at[step],
            chain_recv.at[piece, of_level, 1 - upward],
            sp,
            tp - 2 + 4 * upward,
            when,
        )

    def gather_plane(step):
        place = step % levels
        for kind in (TO_X, TO_Y, LAST_X, LAST_Y):
            arrive(landed.at[step, kind], plane_recv.at[step, kind])
        low = (
            wide(block(step, sp, 0, half)[...])
            + wide(landed[step, TO_X])
            + wide(landed[step, LAST_Y])
        )
        high = (
            wide(block(step, sp, half, half)[...])
            + wide(landed[step, TO_Y])
            + wide(landed[step, LAST_X])
        )
        plane_sum[step, :half] = low
        plane_sum[step, half:] = high
        if place < levels - 1:

            @pl.when(at_end)
            def _():
                z_send[step, :half] = low.astype(z_send.dtype)
                z_send[step, half:] = high.astype(z_send.dtype)

            chain(step, pl.when(at_end))

    def chained(piece, of_level, way):
        arrive(z_land.at[piece, of_level, way], chain_recv.at[piece, of_level, way])
        return wide(z_land[piece, of_level, way])

    def columns(of_level, of_core, piece):
        return pl.ds(
            pl.multiple_of((of_level * 2 + of_core) * half_cols + piece * cols, 128), cols
        )

    def spread_up(piece, of_level, when):
        view = token_out.at[:, columns(of_level, core, piece)]
        send(view, view, up_send.at[piece, of_level], spread_recv.at[piece, of_level], sp, tp + 2, when)

    def spread_down(piece, of_level, when):
        view = token_out.at[:, columns(of_level, core, piece)]
        send(view, view, down_send.at[piece, of_level], spread_recv.at[piece, of_level], sp, tp - 2, when)

    def quarter(of_sp, of_core, piece):
        return quarter_out.at[
            pl.ds(pl.multiple_of(of_sp * rows, 128), rows),
            pl.ds(pl.multiple_of(of_core * half_cols + piece * cols, 128), cols),
        ]

    def share(piece, of_level, valid):
        view = token_out.at[:, columns(of_level, core, piece)]
        send(
            view,
            quarter(sp, core, piece),
            quarter_send.at[piece, of_level],
            quarter_recv.at[piece, sp],
            of_level,
            tp,
            pl.when(valid & (of_level != sp)),
        )
        send(
            view,
            view,
            peer_send.at[piece, of_level],
            peer_recv.at[piece, of_level],
            sp,
            peer,
            pl.when(valid),
        )

    def settle(step):
        piece, place = step // levels, step % levels
        if place < levels - 1:
            of_level = level_at(level, place)
            upward = jnp.where(of_level > level, jnp.int32(1), jnp.int32(0))

            @pl.when(jnp.logical_not(at_end))
            def _():
                total = plane_sum[step] + chained(piece, of_level, 1 - upward)
                z_send[step] = total.astype(z_send.dtype)

            chain(step, pl.when(jnp.logical_not(at_end)))
            return
        span = slice(piece * cols, (piece + 1) * cols)
        plane_sum[step] += wide(cot_in[:, span])

        @pl.when(level > 0)
        def _():
            plane_sum[step] += chained(piece, level, 0)

        @pl.when(level < levels - 1)
        def _():
            plane_sum[step] += chained(piece, level, 1)

        result = plane_sum[step].astype(own_out.dtype)
        own_out[:, span] = result
        token_out[:, columns(level, core, piece)] = result
        spread_up(piece, level, pl.when(level < levels - 1))
        spread_down(piece, level, pl.when(level > 0))
        share(piece, level, level >= 0)

    def spread(piece, hop):
        for up in (True, False):
            of_level = level - hop if up else level + hop
            valid = of_level >= 0 if up else of_level < levels
            safe = jnp.where(valid, of_level, level)

            @pl.when(valid)
            def _():
                arrive(
                    token_out.at[:, columns(safe, core, piece)], spread_recv.at[piece, safe]
                )

            if up:
                spread_up(piece, safe, pl.when(valid & (level < levels - 1)))
            else:
                spread_down(piece, safe, pl.when(valid & (level > 0)))
            share(piece, safe, valid)

    def mate(piece):
        for of_sp in (beside_x, beside_y, across):
            view = quarter(of_sp, core, piece)
            arrive(view, quarter_recv.at[piece, of_sp])
            send(view, view, mate_send.at[piece, of_sp], mate_recv.at[piece, of_sp], sp, peer)

    def give_act():
        for at, to_sp in enumerate((beside_x, beside_y, across)):
            send(
                act_in,
                act_out.at[:, pl.ds(pl.multiple_of(sp * rows, 128), rows)],
                act_send.at[at],
                act_recv.at[sp],
                to_sp,
                tp,
            )

    form(0)
    for turn in range(1, steps + 6):
        if turn < steps:
            form(turn)
        if 0 <= turn - 1 < steps:
            hand_on(turn - 1)
        if turn - 1 == steps - 1:
            give_act()
        if 0 <= turn - 2 < steps:
            gather_plane(turn - 2)
        if 0 <= turn - 3 < steps:
            settle(turn - 3)
        for piece in range(PIECES):
            hop = turn - (piece * levels + levels - 1 + 3)
            if 1 <= hop < levels:
                spread(piece, hop)
    for piece in range(PIECES):
        mate(piece)

    act_out[:, pl.ds(pl.multiple_of(sp * rows, 128), rows)] = act_in[...]
    for piece in range(PIECES):
        for of_level in range(levels):
            view = token_out.at[:, columns(of_level, 1 - core, piece)]
            arrive(view, peer_recv.at[piece, of_level])
        for of_sp in (beside_x, beside_y, across):
            arrive(quarter(of_sp, 1 - core, piece), mate_recv.at[piece, of_sp])
    for of_sp in (beside_x, beside_y, across):
        arrive(
            act_out.at[:, pl.ds(pl.multiple_of(of_sp * rows, 128), rows)], act_recv.at[of_sp]
        )
    quarter_out[pl.ds(pl.multiple_of(sp * rows, 128), rows), :] = token_out[
        :, pl.ds(pl.multiple_of(sp * 2 * half_cols, 128), 2 * half_cols)
    ]
    for when, finish in sent:
        when(finish)


def reduce_all(back, gate_w, up_w, cotangent, act):
    rows, half_cols = cotangent.shape
    hidden, width = gate_w.shape
    steps, cols, half = PIECES * 4, half_cols // PIECES, rows // 2
    dma = pltpu.SemaphoreType.DMA
    vmem = pl.BlockSpec(memory_space=pltpu.VMEM)
    hbm = pl.BlockSpec(memory_space=pl.ANY)
    narrow = jnp.bfloat16
    return pl.pallas_call(
        reduce_kernel,
        out_shape=(
            jax.ShapeDtypeStruct((rows, half_cols), narrow),
            jax.ShapeDtypeStruct((rows, width), narrow),
            jax.ShapeDtypeStruct((4 * rows, 2 * half_cols), narrow),
            jax.ShapeDtypeStruct((act.shape[0], 4 * rows), narrow),
        ),
        in_specs=[vmem, hbm, hbm, vmem, vmem],
        out_specs=[vmem] * 4,
        scratch_shapes=[
            pltpu.VMEM((4 * rows, 4 * hidden), narrow),
            pltpu.VMEM((4, 4 * hidden, half_cols), narrow),
            pltpu.VMEM((steps, 4 * rows, cols), narrow),
            pltpu.VMEM((steps, 2, half, cols), narrow),
            pltpu.VMEM((steps, 6, half, cols), narrow),
            pltpu.VMEM((steps, rows, cols), jnp.float32),
            pltpu.VMEM((steps, rows, cols), narrow),
            pltpu.VMEM((PIECES, 4, 2, rows, cols), narrow),
            dma((9,)),
            dma((9,)),
            dma((9,)),
            dma((steps, 6)),
            dma((steps, 6)),
            dma((steps,)),
            dma((PIECES, 4, 2)),
            dma((PIECES, 4)),
            dma((PIECES, 4)),
            dma((PIECES, 4)),
            dma((PIECES, 4)),
            dma((PIECES, 4)),
            dma((PIECES, 4)),
            dma((PIECES, 4)),
            dma((PIECES, 4)),
            dma((PIECES, 4)),
            dma((3,)),
            dma((4,)),
        ],
        compiler_params=pltpu.CompilerParams(
            collective_id=1, has_side_effects=True, vmem_limit_bytes=48 * 1024 * 1024
        ),
        name="reduce_all",
    )(back, gate_w, up_w, cotangent, act)


def outer_kernel(hidden_ref, gate_ref, up_ref, state_ref, cot_ref, g_out, u_out, d_out, turned):
    @pl.when(pl.program_id(0) == 0)
    def _():
        turned[0] = hidden_ref[...].T
        turned[1] = gate_ref[...].T
        turned[2] = up_ref[...].T

    d_out[...] = jnp.dot(turned[0], cot_ref[...], preferred_element_type=jnp.float32)
    g_out[...] = jnp.dot(turned[1], state_ref[...], preferred_element_type=jnp.float32)
    u_out[...] = jnp.dot(turned[2], state_ref[...], preferred_element_type=jnp.float32)


def weight_grads(hidden, back_gate, back_up, state, cot):
    rows, units = hidden.shape
    width = state.shape[1]
    tile = min(512, width)
    whole = pl.BlockSpec((rows, units), lambda i: (0, 0))
    tall = pl.BlockSpec((rows, tile), lambda i: (0, i))
    flat = pl.BlockSpec((units, tile), lambda i: (0, i))
    out = jax.ShapeDtypeStruct((units, width), jnp.float32)
    return pl.pallas_call(
        outer_kernel,
        grid=(width // tile,),
        out_shape=(out, out, out),
        in_specs=[whole, whole, whole, tall, tall],
        out_specs=[flat, flat, flat],
        scratch_shapes=[pltpu.VMEM((3, units, rows), jnp.bfloat16)],
        cost_estimate=pl.CostEstimate(
            flops=6 * rows * units * width,
            bytes_accessed=4 * rows * width + 12 * units * width,
            transcendentals=0,
        ),
        name="weight_grads",
    )(hidden, back_gate, back_up, state, cot)


def conv_forward(conv_outer, conv_inner, conv_input, conv_taps):
    tok_count = conv_inner.shape[1]
    taps_count = conv_taps.shape[0]
    rim_width = taps_count - 1
    head_block = from_behind(
        jnp.stack([conv_inner[:, tok_count - rim_width :], conv_input[:, tok_count - rim_width :]]),
        "sp",
        1,
    )
    inner_ext = jnp.concatenate([head_block[0], conv_inner], axis=1).astype(jnp.float32)
    input_ext = jnp.concatenate([head_block[1], conv_input], axis=1).astype(jnp.float32)
    inner_prod = inner_ext * input_ext
    conv_out = jnp.zeros((conv_inner.shape[0], tok_count), jnp.float32)
    for offset in range(taps_count):
        conv_out = (
            conv_out + conv_taps[offset][:, None] * inner_prod[:, offset : offset + tok_count]
        )
    outer_f = conv_outer.astype(jnp.float32)
    mixer_act = (outer_f * conv_out).astype(jnp.bfloat16)
    return conv_out, outer_f, mixer_act


def conv_backward(back_mixer, conv_out, outer_f, conv_inner, conv_input, conv_taps):
    tok_count = conv_inner.shape[1]
    taps_count = conv_taps.shape[0]
    rim_width = taps_count - 1
    grad_outer = (back_mixer * conv_out).astype(jnp.bfloat16)
    back_conv = back_mixer * outer_f
    tail_back = from_behind(back_conv[:, :rim_width], "sp", -1)
    back_ext = jnp.concatenate([back_conv, tail_back], axis=1)
    back_prod = jnp.zeros_like(back_conv)
    for offset in range(taps_count):
        shift_by = rim_width - offset
        back_prod = (
            back_prod + conv_taps[offset][:, None] * back_ext[:, shift_by : shift_by + tok_count]
        )
    grad_inner = (back_prod * conv_input.astype(jnp.float32)).astype(jnp.bfloat16)
    grad_input = (back_prod * conv_inner.astype(jnp.float32)).astype(jnp.bfloat16)
    return grad_outer, grad_inner, grad_input


def whole_rows(
    conv_outer,
    conv_inner,
    conv_input,
    conv_taps,
    out_proj,
    mixed_state,
    route_ids,
    route_weights,
    w_gate,
    w_up,
    w_down,
    cotangent,
):
    experts = w_gate.shape[0] * lax.axis_size("sp")
    gate_w, up_w, down_w = w_gate[0], w_up[0], w_down[0]
    choice = route_ids[:, :, None] == jnp.arange(experts, dtype=jnp.int32)[None, None, :]
    scale_of = jnp.sum(jnp.where(choice, route_weights[:, :, None], 0.0), axis=1).T
    scales = lax.all_to_all(
        scale_of[:, None], "sp", split_axis=0, concat_axis=1, tiled=True
    ).reshape(-1, 1)
    conv_out, outer_f, mixer_act = conv_forward(conv_outer, conv_inner, conv_input, conv_taps)
    cot_all, rows_in = gather_all(cotangent, mixed_state)
    gate_pre = jnp.einsum("rd,fd->rf", rows_in, gate_w, preferred_element_type=jnp.float32)
    up_pre = jnp.einsum("rd,fd->rf", rows_in, up_w, preferred_element_type=jnp.float32)
    back_hidden = scales * jnp.einsum(
        "rd,fd->rf", cot_all, down_w, preferred_element_type=jnp.float32
    )
    sig_gate = jax.nn.sigmoid(gate_pre)
    silu_gate = gate_pre * sig_gate
    hidden = (scales * (silu_gate * up_pre)).astype(jnp.bfloat16)
    back_gate = (back_hidden * up_pre * sig_gate * (1.0 + gate_pre * (1.0 - sig_gate))).astype(
        jnp.bfloat16
    )
    back_up = (back_hidden * silu_gate).astype(jnp.bfloat16)
    grad_mixed, tokens, quarter, act_all = reduce_all(
        jnp.concatenate([back_gate, back_up], axis=1), gate_w, up_w, cotangent, mixer_act
    )
    back_mixer = jnp.einsum("cd,td->ct", out_proj, tokens, preferred_element_type=jnp.float32)
    grad_proj = jnp.dot(act_all, quarter, preferred_element_type=jnp.float32)
    grad_gate_e, grad_up_e, grad_down_e = weight_grads(
        hidden, back_gate, back_up, rows_in, cot_all
    )
    grad_outer, grad_inner, grad_input = conv_backward(
        back_mixer, conv_out, outer_f, conv_inner, conv_input, conv_taps
    )
    return (
        grad_gate_e[None],
        grad_up_e[None],
        grad_down_e[None],
        grad_mixed,
        grad_proj,
        grad_outer,
        grad_inner,
        grad_input,
    )


def routed_rows(
    conv_outer,
    conv_inner,
    conv_input,
    conv_taps,
    out_proj,
    mixed_state,
    route_ids,
    route_weights,
    w_gate,
    w_up,
    w_down,
    cotangent,
):
    tok_count = mixed_state.shape[0]
    col_count = mixed_state.shape[1]
    top_count = route_ids.shape[1]
    sp_size = lax.axis_size("sp")
    local_experts = w_gate.shape[0]
    experts = local_experts * sp_size
    capacity = 4 * tok_count // experts
    flat_ids = route_ids.reshape(-1)
    onehot = (flat_ids[:, None] == jnp.arange(experts, dtype=jnp.int32)[None, :]).astype(jnp.int32)
    slot_pos = jnp.sum(jnp.cumsum(onehot, axis=0) * onehot, axis=1) - 1
    slot_dest = flat_ids * capacity + slot_pos
    token_of = jnp.arange(flat_ids.shape[0], dtype=jnp.int32) // top_count
    scale_flat = route_weights.reshape(-1)[:, None]

    def pack_rows(rows):
        buffer = jnp.zeros((experts * capacity, rows.shape[1]), rows.dtype).at[slot_dest].set(rows)
        return buffer.reshape(sp_size, local_experts, capacity, rows.shape[1])

    sent_state = pack_rows(mixed_state[token_of])
    sent_grad = pack_rows(
        (cotangent[token_of].astype(jnp.float32) * scale_flat).astype(jnp.bfloat16)
    )
    recv_state, recv_grad = (
        lax.all_to_all(sent_state, "sp", split_axis=0, concat_axis=0, tiled=True),
        lax.all_to_all(sent_grad, "sp", split_axis=0, concat_axis=0, tiled=True),
    )
    state_rows, grad_rows = (
        lax.all_gather(recv_state[:, 0], "tp", axis=2, tiled=True),
        lax.all_gather(recv_grad[:, 0], "tp", axis=2, tiled=True),
    )
    width = state_rows.shape[2]
    rows_in = state_rows.reshape(-1, width)
    rows_grad = grad_rows.reshape(-1, width)
    partial_value, grad_gate_e, grad_up_e, grad_down_e = expert_step(
        rows_in, rows_grad, w_gate[0], w_up[0], w_down[0]
    )
    summed = lax.psum_scatter(partial_value, "tp", scatter_dimension=1, tiled=True)
    back_rows = summed.reshape(sp_size, capacity, col_count)
    arrived = lax.all_to_all(
        back_rows[:, None], "sp", split_axis=0, concat_axis=0, tiled=True
    ).reshape(experts * capacity, col_count)
    picked = arrived[slot_dest].astype(jnp.float32).reshape(tok_count, top_count, col_count)
    grad_mixed = (cotangent.astype(jnp.float32) + jnp.sum(picked, axis=1)).astype(jnp.bfloat16)
    conv_out, outer_f, mixer_act = conv_forward(conv_outer, conv_inner, conv_input, conv_taps)
    full_back = lax.all_gather(grad_mixed, "tp", axis=1, tiled=True)
    back_mixer = jnp.einsum("cd,td->ct", out_proj, full_back, preferred_element_type=jnp.float32)
    proj_term = jnp.dot(mixer_act, full_back, preferred_element_type=jnp.float32)
    grad_proj = lax.psum_scatter(
        proj_term.astype(jnp.bfloat16), "sp", scatter_dimension=1, tiled=True
    ).astype(jnp.float32)
    grad_outer, grad_inner, grad_input = conv_backward(
        back_mixer, conv_out, outer_f, conv_inner, conv_input, conv_taps
    )
    return (
        grad_gate_e[None],
        grad_up_e[None],
        grad_down_e[None],
        grad_mixed,
        grad_proj,
        grad_outer,
        grad_inner,
        grad_input,
    )


def shards(*operands):
    mixed_state, cotangent, w_gate = operands[5], operands[11], operands[8]
    tok_count = mixed_state.shape[0]
    sp_size, tp_size = lax.axis_size("sp"), lax.axis_size("tp")
    capacity = 4 * tok_count // (w_gate.shape[0] * sp_size)
    small = capacity == tok_count and sp_size == 4 and tp_size == 8
    return (whole_rows if small else routed_rows)(*operands)


def solution(mesh):
    placed = (
        P("tp", "sp"),
        P("tp", "sp"),
        P("tp", "sp"),
        P(None, "tp"),
        P("tp", None),
        P("sp", "tp"),
        P("sp", None),
        P("sp", None),
        P("sp", "tp", None),
        P("sp", "tp", None),
        P("sp", "tp", None),
        P("sp", "tp"),
    )
    return jax.shard_map(
        shards,
        mesh=mesh,
        in_specs=placed,
        out_specs=(
            P("sp", "tp", None),
            P("sp", "tp", None),
            P("sp", "tp", None),
            P("sp", "tp"),
            P("tp", "sp"),
            P("tp", "sp"),
            P("tp", "sp"),
            P("tp", "sp"),
        ),
        check_vma=False,
    )
```

```python
import functools

import jax
import jax.numpy as jnp
from jax import lax
from jax.experimental import pallas as pl
from jax.experimental.pallas import tpu as pltpu
from jax.sharding import PartitionSpec as P


def from_behind(value, axis, steps):
    count = lax.axis_size(axis)
    first, last = (max(0, -steps), min(count, count - steps))
    return lax.ppermute(value, axis, [(source, source + steps) for source in range(first, last)])


def row_back_kernel(gate_ref, up_ref, gate_w_ref, up_w_ref, out_ref):
    total = jnp.dot(gate_ref[...], gate_w_ref[...], preferred_element_type=jnp.float32)
    total += jnp.dot(up_ref[...], up_w_ref[...], preferred_element_type=jnp.float32)
    out_ref[...] = total.astype(out_ref.dtype)


def row_back(back_gate, back_up, gate_w, up_w):
    rows, hidden = back_gate.shape
    width = gate_w.shape[1]
    tile = min(512, width)
    left = pl.BlockSpec((rows, hidden), lambda i: (0, 0))
    right = pl.BlockSpec((hidden, tile), lambda i: (0, i))
    return pl.pallas_call(
        row_back_kernel,
        grid=(width // tile,),
        out_shape=jax.ShapeDtypeStruct((rows, width), jnp.bfloat16),
        in_specs=[left, left, right, right],
        out_specs=pl.BlockSpec((rows, tile), lambda i: (0, i)),
        cost_estimate=pl.CostEstimate(
            flops=4 * rows * hidden * width,
            bytes_accessed=2 * (2 * rows * hidden + 2 * hidden * width + rows * width),
            transcendentals=0,
        ),
        name="row_back",
    )(back_gate, back_up, gate_w, up_w)


def expert_step(rows_in, rows_grad, gate_w, up_w, down_w):
    gate_pre = jnp.einsum("rd,fd->rf", rows_in, gate_w, preferred_element_type=jnp.float32)
    up_pre = jnp.einsum("rd,fd->rf", rows_in, up_w, preferred_element_type=jnp.float32)
    sig_gate = jax.nn.sigmoid(gate_pre)
    silu_gate = gate_pre * sig_gate
    hidden = (silu_gate * up_pre).astype(jnp.bfloat16)
    back_hidden = jnp.einsum("rd,fd->rf", rows_grad, down_w, preferred_element_type=jnp.float32)
    back_gate = (back_hidden * up_pre * sig_gate * (1.0 + gate_pre * (1.0 - sig_gate))).astype(
        jnp.bfloat16
    )
    back_up = (back_hidden * silu_gate).astype(jnp.bfloat16)
    grad_down_e = jnp.einsum("rf,rd->fd", hidden, rows_grad, preferred_element_type=jnp.float32)
    grad_gate_e = jnp.einsum("rf,rd->fd", back_gate, rows_in, preferred_element_type=jnp.float32)
    grad_up_e = jnp.einsum("rf,rd->fd", back_up, rows_in, preferred_element_type=jnp.float32)
    partial_value = row_back(back_gate, back_up, gate_w, up_w)
    return (partial_value, grad_gate_e, grad_up_e, grad_down_e)


COLUMN, BY_X, BY_Y, CORNER, Z_CORNER, PRODUCT = range(6)
FAR, NEAR, IN_X, IN_Y, HALF_X, HALF_Y, IN_CORNER, PEER = range(8)
KINDS = PEER + 4
LEVELS = 4
END_ORDER = (
    (0, 1, 0), (0, 0, 0), (1, 1, 0), (2, 1, 0), (0, 1, 1), (1, 0, 0),
    (2, 0, 0), (0, 0, 1), (3, 1, 0), (5, 1, 0), (0, 1, 2), (1, 1, 1),
    (2, 1, 1), (3, 0, 0), (0, 0, 2), (5, 0, 0), (1, 0, 1), (2, 0, 1),
    (0, 1, 3), (1, 1, 2), (2, 1, 2), (4, 1, 1), (5, 1, 1), (1, 0, 2),
    (2, 0, 2), (0, 0, 3), (1, 1, 3), (2, 1, 3), (4, 0, 1), (3, 1, 2),
    (5, 0, 1), (5, 1, 2), (4, 1, 3), (3, 0, 2), (5, 1, 3), (5, 0, 2),
    (1, 0, 3), (2, 0, 3), (4, 0, 3), (5, 0, 3),
)
INNER_ORDER = (
    (0, 1, 1), (0, 0, 1), (0, 1, 0), (1, 1, 1), (2, 1, 1), (0, 1, 2),
    (0, 0, 0), (1, 0, 1), (2, 0, 1), (0, 0, 2), (1, 1, 0), (2, 1, 0),
    (0, 1, 3), (3, 1, 1), (5, 1, 1), (4, 1, 0), (0, 0, 3), (5, 1, 0),
    (1, 1, 2), (2, 1, 2), (4, 0, 0), (1, 0, 0), (2, 0, 0), (5, 0, 0),
    (3, 0, 1), (4, 1, 3), (5, 0, 1), (1, 0, 2), (2, 0, 2), (4, 0, 3),
    (1, 1, 3), (2, 1, 3), (5, 1, 3), (1, 0, 3), (2, 0, 3), (5, 0, 3),
    (3, 1, 2), (5, 1, 2), (3, 0, 2), (5, 0, 2),
)


def gather_kernel(
    cot_in,
    state_in,
    scale_in,
    inner_in,
    input_in,
    gate_in,
    up_in,
    down_in,
    cot_out,
    state_out,
    hidden_out,
    back_out,
    head_out,
    cot_rows,
    state_rows,
    gate_w,
    up_w,
    down_w,
    gate_acc,
    up_acc,
    back_acc,
    scale_land,
    own_sem,
    weight_sem,
    store_sem,
    small_send,
    small_recv,
    send_sem,
    recv_sem,
):
    sp, tp = lax.axis_index("sp"), lax.axis_index("tp")
    levels = LEVELS
    level, core = tp // 2, tp % 2
    beside_x = sp + 1 - 2 * (sp % 2)
    beside_y = (sp + 2) % 4
    across = 3 - sp
    peer = tp + 1 - 2 * core
    rows, cols = cot_in.shape
    half = rows // 2
    ins, outs, stores = (cot_in, state_in), (cot_rows, state_rows), (cot_out, state_out)
    at_end = (level == 0) | (level == levels - 1)

    barrier = pltpu.get_barrier_semaphore()

    def greet(to_sp, to_tp):
        pl.semaphore_signal(
            barrier,
            inc=1,
            device_id=(to_sp, to_tp),
            device_id_type=pl.DeviceIdType.MESH,
        )

    greet(beside_x, tp)
    greet(beside_y, tp)
    greet(across, tp)
    greet(sp, peer)
    pl.when(level > 0)(lambda: greet(sp, tp - 2))
    pl.when(level < levels - 1)(lambda: greet(sp, tp + 2))
    weight_copies = [
        pltpu.make_async_copy(source, target, weight_sem.at[at])
        for at, (source, target) in enumerate(
            ((gate_in, gate_w), (up_in, up_w), (down_in, down_w))
        )
    ]
    for copy in weight_copies:
        copy.start()
    pl.semaphore_wait(barrier, 6 - jnp.where(at_end, jnp.int32(1), jnp.int32(0)))

    def block(array, of_sp, of_level, of_core, start=0, size=rows):
        return outs[array].at[
            pl.ds(pl.multiple_of(of_sp * rows + start, 16), size),
            pl.ds(pl.multiple_of((of_level * 2 + of_core) * cols, 128), cols),
        ]

    def copy_to(source, target, send, recv, to_sp, to_tp):
        return pltpu.make_async_remote_copy(
            src_ref=source,
            dst_ref=target,
            send_sem=send,
            recv_sem=recv,
            device_id=(to_sp, to_tp),
            device_id_type=pl.DeviceIdType.MESH,
        )

    def remote(array, kind, of_level, source, target, to_sp, to_tp, lands=None):
        return copy_to(
            source,
            target,
            send_sem.at[array, kind, of_level],
            recv_sem.at[array, kind if lands is None else lands, of_level],
            to_sp,
            to_tp,
        )

    def scale_copy(at, to_sp):
        return copy_to(
            scale_in.at[to_sp],
            scale_land.at[sp],
            small_send.at[at],
            small_recv.at[sp],
            to_sp,
            tp,
        )

    def head_copy(which):
        source = (inner_in, input_in)[which]
        width = source.shape[1]
        return copy_to(
            source.at[:, pl.ds(width - 128, 128)],
            head_out.at[which],
            small_send.at[3 + which],
            small_recv.at[4 + which],
            sp + 1,
            tp,
        )

    others = (beside_x, beside_y, across)
    for at, to_sp in enumerate(others):
        scale_copy(at, to_sp).start()
    scale_land[sp] = scale_in[sp]

    def pass_on(sent, *operands, lands=None):
        def build():
            return remote(*operands, lands=lands)

        build().start()
        sent.append(build)

    def arrive(array, kind, of_level, of_sp, of_core, start=0, size=rows):
        piece = block(array, of_sp, of_level, of_core, start, size)
        remote(array, kind, of_level, piece, piece, sp, peer).wait_recv()

    def inward(array, place, inner, sent):
        of_level = jnp.where(level < levels // 2, place, levels - 1 - place)
        far = tp + jnp.where(level < levels // 2, 2, -2)
        near = 2 * tp - far
        flat = place in ((1, 2) if inner else (0, 2))
        mine = place == inner

        def hand_on(kind, of_sp, to_sp, to_tp, start=0, size=rows, lands=None):
            piece = block(array, of_sp, of_level, core, start, size)
            pass_on(sent, array, kind, of_level, piece, piece, to_sp, to_tp, lands=lands)

        def column():
            target = block(array, sp, of_level, core)
            source = ins[array] if mine else target
            if mine:
                pltpu.make_async_copy(source, target, own_sem.at[array]).start()
            else:
                arrive(array, FAR, of_level, sp, core)

            def give(kind, to_sp, to_tp, lands=None):
                pass_on(sent, array, kind, of_level, source, target, to_sp, to_tp, lands=lands)

            if place <= inner:
                give(FAR, sp, far)
            if inner and place >= inner:
                give(NEAR, sp, near, FAR)
            give(IN_X, beside_x, tp)
            give(IN_Y, beside_y, tp)
            give(PEER, sp, peer)

        def by_x():
            arrive(array, IN_X, of_level, beside_x, core)
            if flat:
                hand_on(HALF_Y, beside_x, beside_y, tp, 0, half)
            hand_on(PEER + 1, beside_x, sp, peer)

        def by_y():
            arrive(array, IN_Y, of_level, beside_y, core)
            if flat:
                hand_on(HALF_X, beside_y, beside_x, tp, half, half)
            hand_on(PEER + 2, beside_y, sp, peer)

        def corner():
            if flat:
                arrive(array, HALF_X, of_level, across, core, half, half)
                arrive(array, HALF_Y, of_level, across, core, 0, half)
            else:
                arrive(array, IN_CORNER, of_level, across, core)
            if place == 0:
                hand_on(IN_CORNER, across, sp, far)
            elif inner and place in (1, 3):
                hand_on(IN_CORNER, across, sp, near)
            hand_on(PEER + 3, across, sp, peer)

        return of_level, mine, (column, by_x, by_y, corner, corner)

    def slab(ref, of_level):
        return ref.at[:, pl.ds(pl.multiple_of(of_level * 2 * cols, 128), 2 * cols)]

    def store(array, of_level):
        return pltpu.make_async_copy(
            slab(outs[array], of_level),
            slab(stores[array], of_level),
            store_sem.at[array, of_level],
        )

    def product(array, of_level, mine, first):
        for at, of_sp in enumerate((sp, beside_x, beside_y, across)):
            arrive(array, PEER + at, of_level, of_sp, 1 - core)
        if mine:
            pltpu.make_async_copy(
                ins[array], block(array, sp, level, core), own_sem.at[array]
            ).wait()
        if first:
            for at in (0, 1) if array == 1 else (2,):
                weight_copies[at].wait()
        store(array, of_level).start()
        pairs = ((gate_w, gate_acc), (up_w, up_acc)) if array == 1 else ((down_w, back_acc),)
        span = pl.ds(pl.multiple_of(of_level * 2 * cols, 128), 2 * cols)

        def one(at, _):
            lines = pl.ds(pl.multiple_of(at * rows, 128), rows)
            for weight, acc in pairs:
                value = lax.dot_general(
                    outs[array][lines, span],
                    weight[:, span],
                    (((1,), (1,)), ((), ())),
                    preferred_element_type=jnp.float32,
                )
                acc[lines, :] = value if first else acc[lines, :] + value
            return 0

        lax.fori_loop(0, 4, one, 0)

    def give_head():
        head_copy(0).start()
        head_copy(1).start()

    def follow(order, inner):
        sent, begun = [], set()
        flats = (1, 2) if inner else (0, 2)
        last = max(
            at
            for at, (kind, _, place) in enumerate(order)
            if kind == COLUMN or (kind in (BY_X, BY_Y) and place in flats)
        )
        for at, (kind, array, place) in enumerate(order):
            if at == last + 1:
                pl.when(sp < 3)(give_head)
            of_level, mine, actions = inward(array, place, inner, sent)
            if kind == PRODUCT:
                product(array, of_level, mine, array not in begun)
                begun.add(array)
            else:
                actions[kind]()
        for build in sent:
            build().wait_send()

    pl.when(at_end)(lambda: follow(END_ORDER, 0))
    pl.when(jnp.logical_not(at_end))(lambda: follow(INNER_ORDER, 1))

    for at, to_sp in enumerate(others):
        copy_to(
            scale_land.at[to_sp],
            scale_land.at[to_sp],
            small_send.at[at],
            small_recv.at[to_sp],
            sp,
            peer,
        ).wait_recv()
    units = hidden_out.shape[1]

    def finish(at, _):
        lines = pl.ds(pl.multiple_of(at * rows, 128), rows)
        scale = jnp.broadcast_to(scale_land[at, 0:1, :], (units, rows)).T
        gate_pre, up_pre = gate_acc[lines, :], up_acc[lines, :]
        sig_gate = 1.0 / (1.0 + jnp.exp(-gate_pre))
        silu_gate = gate_pre * sig_gate
        back_hidden = scale * back_acc[lines, :]
        hidden_out[lines, :] = (scale * (silu_gate * up_pre)).astype(hidden_out.dtype)
        back_out[lines, :units] = (
            back_hidden * up_pre * sig_gate * (1.0 + gate_pre * (1.0 - sig_gate))
        ).astype(back_out.dtype)
        back_out[lines, units:] = (back_hidden * silu_gate).astype(back_out.dtype)
        return 0

    lax.fori_loop(0, 4, finish, 0)

    @pl.when(sp == 0)
    def _():
        head_out[...] = jnp.zeros_like(head_out)

    @pl.when(sp > 0)
    def _():
        for which in range(2):
            copy_to(
                head_out.at[which],
                head_out.at[which],
                small_send.at[3 + which],
                small_recv.at[4 + which],
                sp,
                peer,
            ).wait_recv()

    @pl.when(sp < 3)
    def _():
        head_copy(0).wait_send()
        head_copy(1).wait_send()

    for at, to_sp in enumerate(others):
        scale_copy(at, to_sp).wait_send()
    for array in range(2):
        for of_level in range(levels):
            store(array, of_level).wait()


def gather_all(cotangent, mixed_state, scales, conv_inner, conv_input, gate_w, up_w, down_w):
    rows, cols = cotangent.shape
    units, width = gate_w.shape
    narrow = cotangent.dtype
    dma = pltpu.SemaphoreType.DMA
    vmem = pl.BlockSpec(memory_space=pltpu.VMEM)
    hbm = pl.BlockSpec(memory_space=pl.ANY)
    whole = jax.ShapeDtypeStruct((4 * rows, width), narrow)
    return pl.pallas_call(
        gather_kernel,
        out_shape=(
            whole,
            whole,
            jax.ShapeDtypeStruct((4 * rows, units), narrow),
            jax.ShapeDtypeStruct((4 * rows, 2 * units), narrow),
            jax.ShapeDtypeStruct((2, conv_inner.shape[0], 128), narrow),
        ),
        in_specs=[vmem] * 5 + [hbm] * 3,
        out_specs=[hbm, hbm, vmem, vmem, vmem],
        scratch_shapes=[
            pltpu.VMEM((4 * rows, width), narrow),
            pltpu.VMEM((4 * rows, width), narrow),
            pltpu.VMEM((units, width), narrow),
            pltpu.VMEM((units, width), narrow),
            pltpu.VMEM((units, width), narrow),
            pltpu.VMEM((4 * rows, units), jnp.float32),
            pltpu.VMEM((4 * rows, units), jnp.float32),
            pltpu.VMEM((4 * rows, units), jnp.float32),
            pltpu.VMEM((4, 8, rows), jnp.float32),
            dma((2,)),
            dma((3,)),
            dma((2, LEVELS)),
            dma((5,)),
            dma((6,)),
            dma((2, KINDS, LEVELS)),
            dma((2, KINDS, LEVELS)),
        ],
        compiler_params=pltpu.CompilerParams(
            collective_id=0, has_side_effects=True, vmem_limit_bytes=63 * 1024 * 1024
        ),
        name="gather_all",
    )(cotangent, mixed_state, scales, conv_inner, conv_input, gate_w, up_w, down_w)


PIECES = 2
TO_X, TO_Y, PASS_X, PASS_Y, LAST_X, LAST_Y = range(6)


def level_at(level, place):
    inner = (0, 3, 1, 2)[place]
    high = jnp.where((level == 0) | (level == 3), place, inner)
    return jnp.where(level >= 2, high, 3 - high)


def reduce_kernel(
    back_in,
    gate_in,
    up_in,
    cot_in,
    act_in,
    own_out,
    token_out,
    quarter_out,
    act_out,
    back,
    weights,
    part,
    passed,
    landed,
    plane_sum,
    z_send,
    z_land,
    own_sem,
    swap_send,
    swap_recv,
    plane_send,
    plane_recv,
    chain_send,
    chain_recv,
    up_send,
    down_send,
    spread_recv,
    peer_send,
    peer_recv,
    quarter_send,
    quarter_recv,
    mate_send,
    mate_recv,
    act_send,
    act_recv,
):
    sp, tp = lax.axis_index("sp"), lax.axis_index("tp")
    level, core = tp // 2, tp % 2
    beside_x = sp + 1 - 2 * (sp % 2)
    beside_y = (sp + 2) % 4
    across = 3 - sp
    peer = tp + 1 - 2 * core
    levels = 4
    rows, half_cols = cot_in.shape
    cols = half_cols // PIECES
    half = rows // 2
    hidden = gate_in.shape[0]
    steps = PIECES * levels
    at_end = (level == 0) | (level == levels - 1)

    barrier = pltpu.get_barrier_semaphore()

    def greet(to_sp, to_tp):
        pl.semaphore_signal(
            barrier,
            inc=1,
            device_id=(to_sp, to_tp),
            device_id_type=pl.DeviceIdType.MESH,
        )

    greet(beside_x, tp)
    greet(beside_y, tp)
    greet(across, tp)
    greet(sp, peer)
    pl.when(level > 0)(lambda: greet(sp, tp - 2))
    pl.when(level < levels - 1)(lambda: greet(sp, tp + 2))
    pl.semaphore_wait(barrier, 6 - jnp.where(at_end, jnp.int32(1), jnp.int32(0)))

    sent = []

    def always(action):
        action()

    def remote(source, target, send, recv, to_sp, to_tp):
        return pltpu.make_async_remote_copy(
            src_ref=source,
            dst_ref=target,
            send_sem=send,
            recv_sem=recv,
            device_id=(to_sp, to_tp),
            device_id_type=pl.DeviceIdType.MESH,
        )

    def send(source, target, send_sem, recv_sem, to_sp, to_tp, when=always):
        def build():
            return remote(source, target, send_sem, recv_sem, to_sp, to_tp)

        when(lambda: build().start())
        sent.append((when, lambda: build().wait_send()))

    def arrive(piece, recv_sem):
        remote(piece, piece, act_send.at[0], recv_sem, sp, peer).wait_recv()

    mine = pl.ds(0, 2 * hidden)
    send(back_in, back.at[:, pl.ds(2 * hidden, 2 * hidden)], swap_send.at[0], swap_recv.at[0], sp, peer)
    pltpu.make_async_copy(back_in, back.at[:, mine], own_sem.at[0]).start()

    def own_weights(place, which):
        of_level = level_at(level, place)
        source = (gate_in, up_in)[which].at[
            :, pl.ds(pl.multiple_of((of_level * 2 + core) * half_cols, 128), half_cols)
        ]
        target = weights.at[place, pl.ds(which * hidden, hidden)]
        return pltpu.make_async_copy(source, target, own_sem.at[1 + 2 * place + which])

    for place in range(levels):
        for which in range(2):
            of_level = level_at(level, place)
            send(
                (gate_in, up_in)[which].at[
                    :, pl.ds(pl.multiple_of((of_level * 2 + 1 - core) * half_cols, 128), half_cols)
                ],
                weights.at[place, pl.ds((2 + which) * hidden, hidden)],
                swap_send.at[1 + 2 * place + which],
                swap_recv.at[1 + 2 * place + which],
                sp,
                peer,
            )
            own_weights(place, which).start()

    def block(step, of_sp, start, size):
        return part.at[step, pl.ds(pl.multiple_of(of_sp * rows + start, 128), size)]

    def plane(step, kind, source, to_sp):
        send(
            source,
            landed.at[step, kind],
            plane_send.at[step, kind],
            plane_recv.at[step, kind],
            to_sp,
            tp,
        )

    def form(step):
        piece, place = step // levels, step % levels
        if step < levels:
            for which in range(2):
                own_weights(place, which).wait()
                arrive(
                    weights.at[place, pl.ds((2 + which) * hidden, hidden)],
                    swap_recv.at[1 + 2 * place + which],
                )
        if step == 0:
            pltpu.make_async_copy(back_in, back.at[:, mine], own_sem.at[0]).wait()
            arrive(back.at[:, pl.ds(2 * hidden, 2 * hidden)], swap_recv.at[0])

        def one(at, _):
            span = pl.ds(pl.multiple_of(at * rows, 128), rows)
            part[step, span, :] = jnp.dot(
                back[span, :],
                weights[place, :, piece * cols : (piece + 1) * cols],
                preferred_element_type=jnp.float32,
            ).astype(part.dtype)
            return 0

        lax.fori_loop(0, 4, one, 0)
        plane(step, PASS_X, block(step, across, 0, half), beside_x)
        plane(step, PASS_Y, block(step, across, half, half), beside_y)
        plane(step, TO_X, block(step, beside_x, 0, half), beside_x)
        plane(step, TO_Y, block(step, beside_y, half, half), beside_y)

    def wide(value):
        return value.astype(jnp.float32)

    def hand_on(step):
        arrive(landed.at[step, PASS_X], plane_recv.at[step, PASS_X])
        passed[step, 0] = (
            wide(block(step, beside_y, 0, half)[...]) + wide(landed[step, PASS_X])
        ).astype(passed.dtype)
        plane(step, LAST_Y, passed.at[step, 0], beside_y)
        arrive(landed.at[step, PASS_Y], plane_recv.at[step, PASS_Y])
        passed[step, 1] = (
            wide(block(step, beside_x, half, half)[...]) + wide(landed[step, PASS_Y])
        ).astype(passed.dtype)
        plane(step, LAST_X, passed.at[step, 1], beside_x)

    def chain(step, when):
        piece, place = step // levels, step % levels
        of_level = level_at(level, place)
        upward = jnp.where(of_level > level, jnp.int32(1), jnp.int32(0))
        send(
            z_send.at[step],
            z_land.at[piece, of_level, 1 - upward],
            chain_send.at[step],
            chain_recv.at[piece, of_level, 1 - upward],
            sp,
            tp - 2 + 4 * upward,
            when,
        )

    def gather_plane(step):
        place = step % levels
        for kind in (TO_X, TO_Y, LAST_X, LAST_Y):
            arrive(landed.at[step, kind], plane_recv.at[step, kind])
        low = (
            wide(block(step, sp, 0, half)[...])
            + wide(landed[step, TO_X])
            + wide(landed[step, LAST_Y])
        )
        high = (
            wide(block(step, sp, half, half)[...])
            + wide(landed[step, TO_Y])
            + wide(landed[step, LAST_X])
        )
        plane_sum[step, :half] = low
        plane_sum[step, half:] = high
        if place < levels - 1:

            @pl.when(at_end)
            def _():
                z_send[step, :half] = low.astype(z_send.dtype)
                z_send[step, half:] = high.astype(z_send.dtype)

            chain(step, pl.when(at_end))

    def chained(piece, of_level, way):
        arrive(z_land.at[piece, of_level, way], chain_recv.at[piece, of_level, way])
        return wide(z_land[piece, of_level, way])

    def columns(of_level, of_core, piece):
        return pl.ds(
            pl.multiple_of((of_level * 2 + of_core) * half_cols + piece * cols, 128), cols
        )

    def spread_up(piece, of_level, when):
        view = token_out.at[:, columns(of_level, core, piece)]
        send(view, view, up_send.at[piece, of_level], spread_recv.at[piece, of_level], sp, tp + 2, when)

    def spread_down(piece, of_level, when):
        view = token_out.at[:, columns(of_level, core, piece)]
        send(view, view, down_send.at[piece, of_level], spread_recv.at[piece, of_level], sp, tp - 2, when)

    def quarter(of_sp, of_core, piece):
        return quarter_out.at[
            pl.ds(pl.multiple_of(of_sp * rows, 128), rows),
            pl.ds(pl.multiple_of(of_core * half_cols + piece * cols, 128), cols),
        ]

    def share(piece, of_level, valid):
        view = token_out.at[:, columns(of_level, core, piece)]
        send(
            view,
            quarter(sp, core, piece),
            quarter_send.at[piece, of_level],
            quarter_recv.at[piece, sp],
            of_level,
            tp,
            pl.when(valid & (of_level != sp)),
        )
        send(
            view,
            view,
            peer_send.at[piece, of_level],
            peer_recv.at[piece, of_level],
            sp,
            peer,
            pl.when(valid),
        )

    def settle(step):
        piece, place = step // levels, step % levels
        if place < levels - 1:
            of_level = level_at(level, place)
            upward = jnp.where(of_level > level, jnp.int32(1), jnp.int32(0))

            @pl.when(jnp.logical_not(at_end))
            def _():
                total = plane_sum[step] + chained(piece, of_level, 1 - upward)
                z_send[step] = total.astype(z_send.dtype)

            chain(step, pl.when(jnp.logical_not(at_end)))
            return
        span = slice(piece * cols, (piece + 1) * cols)
        plane_sum[step] += wide(cot_in[:, span])

        @pl.when(level > 0)
        def _():
            plane_sum[step] += chained(piece, level, 0)

        @pl.when(level < levels - 1)
        def _():
            plane_sum[step] += chained(piece, level, 1)

        result = plane_sum[step].astype(own_out.dtype)
        own_out[:, span] = result
        token_out[:, columns(level, core, piece)] = result
        spread_up(piece, level, pl.when(level < levels - 1))
        spread_down(piece, level, pl.when(level > 0))
        share(piece, level, level >= 0)

    def spread(piece, hop):
        for up in (True, False):
            of_level = level - hop if up else level + hop
            valid = of_level >= 0 if up else of_level < levels
            safe = jnp.where(valid, of_level, level)

            @pl.when(valid)
            def _():
                arrive(
                    token_out.at[:, columns(safe, core, piece)], spread_recv.at[piece, safe]
                )

            if up:
                spread_up(piece, safe, pl.when(valid & (level < levels - 1)))
            else:
                spread_down(piece, safe, pl.when(valid & (level > 0)))
            share(piece, safe, valid)

    def mate(piece):
        for of_sp in (beside_x, beside_y, across):
            view = quarter(of_sp, core, piece)
            arrive(view, quarter_recv.at[piece, of_sp])
            send(view, view, mate_send.at[piece, of_sp], mate_recv.at[piece, of_sp], sp, peer)

    def give_act():
        for at, to_sp in enumerate((beside_x, beside_y, across)):
            send(
                act_in,
                act_out.at[:, pl.ds(pl.multiple_of(sp * rows, 128), rows)],
                act_send.at[at],
                act_recv.at[sp],
                to_sp,
                tp,
            )

    form(0)
    for turn in range(1, steps + 6):
        if turn < steps:
            form(turn)
        if 0 <= turn - 1 < steps:
            hand_on(turn - 1)
        if turn - 1 == steps - 1:
            give_act()
        if 0 <= turn - 2 < steps:
            gather_plane(turn - 2)
        if 0 <= turn - 3 < steps:
            settle(turn - 3)
        for piece in range(PIECES):
            hop = turn - (piece * levels + levels - 1 + 3)
            if 1 <= hop < levels:
                spread(piece, hop)
    for piece in range(PIECES):
        mate(piece)

    act_out[:, pl.ds(pl.multiple_of(sp * rows, 128), rows)] = act_in[...]
    for piece in range(PIECES):
        for of_level in range(levels):
            view = token_out.at[:, columns(of_level, 1 - core, piece)]
            arrive(view, peer_recv.at[piece, of_level])
        for of_sp in (beside_x, beside_y, across):
            arrive(quarter(of_sp, 1 - core, piece), mate_recv.at[piece, of_sp])
    for of_sp in (beside_x, beside_y, across):
        arrive(
            act_out.at[:, pl.ds(pl.multiple_of(of_sp * rows, 128), rows)], act_recv.at[of_sp]
        )
    quarter_out[pl.ds(pl.multiple_of(sp * rows, 128), rows), :] = token_out[
        :, pl.ds(pl.multiple_of(sp * 2 * half_cols, 128), 2 * half_cols)
    ]
    for when, finish in sent:
        when(finish)


def reduce_all(back, gate_w, up_w, cotangent, act):
    rows, half_cols = cotangent.shape
    hidden, width = gate_w.shape
    steps, cols, half = PIECES * 4, half_cols // PIECES, rows // 2
    dma = pltpu.SemaphoreType.DMA
    vmem = pl.BlockSpec(memory_space=pltpu.VMEM)
    hbm = pl.BlockSpec(memory_space=pl.ANY)
    narrow = jnp.bfloat16
    return pl.pallas_call(
        reduce_kernel,
        out_shape=(
            jax.ShapeDtypeStruct((rows, half_cols), narrow),
            jax.ShapeDtypeStruct((rows, width), narrow),
            jax.ShapeDtypeStruct((4 * rows, 2 * half_cols), narrow),
            jax.ShapeDtypeStruct((act.shape[0], 4 * rows), narrow),
        ),
        in_specs=[vmem, hbm, hbm, vmem, vmem],
        out_specs=[vmem] * 4,
        scratch_shapes=[
            pltpu.VMEM((4 * rows, 4 * hidden), narrow),
            pltpu.VMEM((4, 4 * hidden, half_cols), narrow),
            pltpu.VMEM((steps, 4 * rows, cols), narrow),
            pltpu.VMEM((steps, 2, half, cols), narrow),
            pltpu.VMEM((steps, 6, half, cols), narrow),
            pltpu.VMEM((steps, rows, cols), jnp.float32),
            pltpu.VMEM((steps, rows, cols), narrow),
            pltpu.VMEM((PIECES, 4, 2, rows, cols), narrow),
            dma((9,)),
            dma((9,)),
            dma((9,)),
            dma((steps, 6)),
            dma((steps, 6)),
            dma((steps,)),
            dma((PIECES, 4, 2)),
            dma((PIECES, 4)),
            dma((PIECES, 4)),
            dma((PIECES, 4)),
            dma((PIECES, 4)),
            dma((PIECES, 4)),
            dma((PIECES, 4)),
            dma((PIECES, 4)),
            dma((PIECES, 4)),
            dma((PIECES, 4)),
            dma((3,)),
            dma((4,)),
        ],
        compiler_params=pltpu.CompilerParams(
            collective_id=1, has_side_effects=True, vmem_limit_bytes=48 * 1024 * 1024
        ),
        name="reduce_all",
    )(back, gate_w, up_w, cotangent, act)


def outer_kernel(hidden_ref, back_ref, state_ref, cot_ref, g_out, u_out, d_out, turned):
    units = hidden_ref.shape[1]

    @pl.when(pl.program_id(0) == 0)
    def _():
        turned[0] = hidden_ref[...].T
        turned[1] = back_ref[:, :units].T
        turned[2] = back_ref[:, units:].T

    d_out[...] = jnp.dot(turned[0], cot_ref[...], preferred_element_type=jnp.float32)
    g_out[...] = jnp.dot(turned[1], state_ref[...], preferred_element_type=jnp.float32)
    u_out[...] = jnp.dot(turned[2], state_ref[...], preferred_element_type=jnp.float32)


def weight_grads(hidden, back, state, cot):
    rows, units = hidden.shape
    width = state.shape[1]
    tile = min(512, width)
    whole = pl.BlockSpec((rows, units), lambda i: (0, 0))
    double = pl.BlockSpec((rows, 2 * units), lambda i: (0, 0))
    tall = pl.BlockSpec((rows, tile), lambda i: (0, i))
    flat = pl.BlockSpec((units, tile), lambda i: (0, i))
    out = jax.ShapeDtypeStruct((units, width), jnp.float32)
    return pl.pallas_call(
        outer_kernel,
        grid=(width // tile,),
        out_shape=(out, out, out),
        in_specs=[whole, double, tall, tall],
        out_specs=[flat, flat, flat],
        scratch_shapes=[pltpu.VMEM((3, units, rows), jnp.bfloat16)],
        cost_estimate=pl.CostEstimate(
            flops=6 * rows * units * width,
            bytes_accessed=4 * rows * width + 12 * units * width,
            transcendentals=0,
        ),
        name="weight_grads",
    )(hidden, back, state, cot)


def conv_head(conv_inner, conv_input, rim_width):
    return from_behind(jnp.stack([conv_inner[:, -rim_width:], conv_input[:, -rim_width:]]), "sp", 1)


def conv_forward(conv_outer, conv_inner, conv_input, conv_taps, head_block):
    tok_count = conv_inner.shape[1]
    taps_count = conv_taps.shape[0]
    inner_ext = jnp.concatenate([head_block[0], conv_inner], axis=1).astype(jnp.float32)
    input_ext = jnp.concatenate([head_block[1], conv_input], axis=1).astype(jnp.float32)
    inner_prod = inner_ext * input_ext
    conv_out = jnp.zeros((conv_inner.shape[0], tok_count), jnp.float32)
    for offset in range(taps_count):
        conv_out = (
            conv_out + conv_taps[offset][:, None] * inner_prod[:, offset : offset + tok_count]
        )
    outer_f = conv_outer.astype(jnp.float32)
    mixer_act = (outer_f * conv_out).astype(jnp.bfloat16)
    return conv_out, outer_f, mixer_act


def conv_backward(back_mixer, conv_out, outer_f, conv_inner, conv_input, conv_taps):
    tok_count = conv_inner.shape[1]
    taps_count = conv_taps.shape[0]
    rim_width = taps_count - 1
    grad_outer = (back_mixer * conv_out).astype(jnp.bfloat16)
    back_conv = back_mixer * outer_f
    tail_back = from_behind(back_conv[:, :rim_width], "sp", -1)
    back_ext = jnp.concatenate([back_conv, tail_back], axis=1)
    back_prod = jnp.zeros_like(back_conv)
    for offset in range(taps_count):
        shift_by = rim_width - offset
        back_prod = (
            back_prod + conv_taps[offset][:, None] * back_ext[:, shift_by : shift_by + tok_count]
        )
    grad_inner = (back_prod * conv_input.astype(jnp.float32)).astype(jnp.bfloat16)
    grad_input = (back_prod * conv_inner.astype(jnp.float32)).astype(jnp.bfloat16)
    return grad_outer, grad_inner, grad_input


def whole_rows(
    conv_outer,
    conv_inner,
    conv_input,
    conv_taps,
    out_proj,
    mixed_state,
    route_ids,
    route_weights,
    w_gate,
    w_up,
    w_down,
    cotangent,
):
    experts = w_gate.shape[0] * lax.axis_size("sp")
    gate_w, up_w, down_w = w_gate[0], w_up[0], w_down[0]
    choice = route_ids[:, :, None] == jnp.arange(experts, dtype=jnp.int32)[None, None, :]
    scale_of = jnp.sum(jnp.where(choice, route_weights[:, :, None], 0.0), axis=1).T
    scales = jnp.broadcast_to(scale_of[:, None, :], (experts, 8, scale_of.shape[1]))
    cot_all, rows_in, hidden, back, head = gather_all(
        cotangent, mixed_state, scales, conv_inner, conv_input, gate_w, up_w, down_w
    )
    rim_width = conv_taps.shape[0] - 1
    conv_out, outer_f, mixer_act = conv_forward(
        conv_outer, conv_inner, conv_input, conv_taps, head[:, :, -rim_width:]
    )
    grad_mixed, tokens, quarter, act_all = reduce_all(back, gate_w, up_w, cotangent, mixer_act)
    back_mixer = jnp.einsum("cd,td->ct", out_proj, tokens, preferred_element_type=jnp.float32)
    grad_proj = jnp.dot(act_all, quarter, preferred_element_type=jnp.float32)
    tokens, hidden = lax.optimization_barrier((tokens, hidden))
    grad_gate_e, grad_up_e, grad_down_e = weight_grads(hidden, back, rows_in, cot_all)
    grad_outer, grad_inner, grad_input = conv_backward(
        back_mixer, conv_out, outer_f, conv_inner, conv_input, conv_taps
    )
    return (
        grad_gate_e[None],
        grad_up_e[None],
        grad_down_e[None],
        grad_mixed,
        grad_proj,
        grad_outer,
        grad_inner,
        grad_input,
    )


def routed_rows(
    conv_outer,
    conv_inner,
    conv_input,
    conv_taps,
    out_proj,
    mixed_state,
    route_ids,
    route_weights,
    w_gate,
    w_up,
    w_down,
    cotangent,
):
    tok_count = mixed_state.shape[0]
    col_count = mixed_state.shape[1]
    top_count = route_ids.shape[1]
    sp_size = lax.axis_size("sp")
    local_experts = w_gate.shape[0]
    experts = local_experts * sp_size
    capacity = 4 * tok_count // experts
    flat_ids = route_ids.reshape(-1)
    onehot = (flat_ids[:, None] == jnp.arange(experts, dtype=jnp.int32)[None, :]).astype(jnp.int32)
    slot_pos = jnp.sum(jnp.cumsum(onehot, axis=0) * onehot, axis=1) - 1
    slot_dest = flat_ids * capacity + slot_pos
    token_of = jnp.arange(flat_ids.shape[0], dtype=jnp.int32) // top_count
    scale_flat = route_weights.reshape(-1)[:, None]

    def pack_rows(rows):
        buffer = jnp.zeros((experts * capacity, rows.shape[1]), rows.dtype).at[slot_dest].set(rows)
        return buffer.reshape(sp_size, local_experts, capacity, rows.shape[1])

    sent_state = pack_rows(mixed_state[token_of])
    sent_grad = pack_rows(
        (cotangent[token_of].astype(jnp.float32) * scale_flat).astype(jnp.bfloat16)
    )
    recv_state, recv_grad = (
        lax.all_to_all(sent_state, "sp", split_axis=0, concat_axis=0, tiled=True),
        lax.all_to_all(sent_grad, "sp", split_axis=0, concat_axis=0, tiled=True),
    )
    state_rows, grad_rows = (
        lax.all_gather(recv_state[:, 0], "tp", axis=2, tiled=True),
        lax.all_gather(recv_grad[:, 0], "tp", axis=2, tiled=True),
    )
    width = state_rows.shape[2]
    rows_in = state_rows.reshape(-1, width)
    rows_grad = grad_rows.reshape(-1, width)
    partial_value, grad_gate_e, grad_up_e, grad_down_e = expert_step(
        rows_in, rows_grad, w_gate[0], w_up[0], w_down[0]
    )
    summed = lax.psum_scatter(partial_value, "tp", scatter_dimension=1, tiled=True)
    back_rows = summed.reshape(sp_size, capacity, col_count)
    arrived = lax.all_to_all(
        back_rows[:, None], "sp", split_axis=0, concat_axis=0, tiled=True
    ).reshape(experts * capacity, col_count)
    picked = arrived[slot_dest].astype(jnp.float32).reshape(tok_count, top_count, col_count)
    grad_mixed = (cotangent.astype(jnp.float32) + jnp.sum(picked, axis=1)).astype(jnp.bfloat16)
    conv_out, outer_f, mixer_act = conv_forward(
        conv_outer,
        conv_inner,
        conv_input,
        conv_taps,
        conv_head(conv_inner, conv_input, conv_taps.shape[0] - 1),
    )
    full_back = lax.all_gather(grad_mixed, "tp", axis=1, tiled=True)
    back_mixer = jnp.einsum("cd,td->ct", out_proj, full_back, preferred_element_type=jnp.float32)
    proj_term = jnp.dot(mixer_act, full_back, preferred_element_type=jnp.float32)
    grad_proj = lax.psum_scatter(
        proj_term.astype(jnp.bfloat16), "sp", scatter_dimension=1, tiled=True
    ).astype(jnp.float32)
    grad_outer, grad_inner, grad_input = conv_backward(
        back_mixer, conv_out, outer_f, conv_inner, conv_input, conv_taps
    )
    return (
        grad_gate_e[None],
        grad_up_e[None],
        grad_down_e[None],
        grad_mixed,
        grad_proj,
        grad_outer,
        grad_inner,
        grad_input,
    )


def shards(*operands):
    mixed_state, cotangent, w_gate = operands[5], operands[11], operands[8]
    tok_count = mixed_state.shape[0]
    sp_size, tp_size = lax.axis_size("sp"), lax.axis_size("tp")
    capacity = 4 * tok_count // (w_gate.shape[0] * sp_size)
    small = capacity == tok_count and sp_size == 4 and tp_size == 8
    return (whole_rows if small else routed_rows)(*operands)


def solution(mesh):
    placed = (
        P("tp", "sp"),
        P("tp", "sp"),
        P("tp", "sp"),
        P(None, "tp"),
        P("tp", None),
        P("sp", "tp"),
        P("sp", None),
        P("sp", None),
        P("sp", "tp", None),
        P("sp", "tp", None),
        P("sp", "tp", None),
        P("sp", "tp"),
    )
    return jax.shard_map(
        shards,
        mesh=mesh,
        in_specs=placed,
        out_specs=(
            P("sp", "tp", None),
            P("sp", "tp", None),
            P("sp", "tp", None),
            P("sp", "tp"),
            P("tp", "sp"),
            P("tp", "sp"),
            P("tp", "sp"),
            P("tp", "sp"),
        ),
        check_vma=False,
    )
```
